32 devices in a mesh: gr: 2 (over y), fs: 4 (over z), tp: 4 (over x, core).
Axes of the slice: x: 2, y: 2, z: 4, core: 2. Of those that a mesh axis runs over, the one named last changes fastest.
Arguments:
- prompt: bfloat16 [4096, 2048], P(('gr', 'fs')), may hold values from -6 to 6
- norm_gain: float32 [2048], P(('gr', 'fs')), may hold values from 0.1 to 1.9
- gate_master: float32 [32, 2048, 1024], P(None, ('gr', 'fs'), 'tp'), may hold values from -6 to 6
- up_master: float32 [32, 2048, 1024], P(None, ('gr', 'fs'), 'tp'), may hold values from -6 to 6
- down_master: float32 [32, 2048, 1024], P(None, ('gr', 'fs'), 'tp'), may hold values from -6 to 6
- routes: int32 [4096, 2], P(('gr', 'fs')), may hold values from 0 to 31, as said below
- route_weights: float32 [4096, 2], P(('gr', 'fs')), may hold values from 0.1 to 0.9
Outputs:
- gate_ready: bfloat16 [32, 2048, 1024], P('fs', None, 'tp')
- up_ready: bfloat16 [32, 2048, 1024], P('fs', None, 'tp')
- down_ready: bfloat16 [32, 2048, 1024], P('fs', None, 'tp')
- blended: bfloat16 [4096, 2048], P(('gr', 'fs'), 'tp')
The draws below stay inside these ranges and needn't reach their ends.
Inputs may be any that keep to these rules, and one draw needn't show every extreme that they name: `routes`: each row names 2 different experts of one group: expert // 8 is the group. In every aligned block of 512 rows (the tokens of one index of gr and fs) half of the rows choose one group, and no expert is named more than 64 times; in every block some expert is named exactly 64 times.
All inputs are finite; a program needn't handle non-finite values.
Results may differ from the reference program's by a relative error of at most 0.015.
Values may be sent and summed in bfloat16 or wider, within the bound.
No kernel may reach another device: no remote copies, remote signals or barrier semaphores. Data moves between devices by JAX's collectives and lax.ppermute only.
A program may use at most 128 MiB of HBM per device.

```python
import jax
import jax.numpy as jnp
from jax import lax

D = 2048
FF = 1024
N_GROUPS = 4
PER_GROUP = 8
TOP = 2
N_EXPERTS = 32
TOK_DEV = 512
CAP = 64
TOKENS = 4096
N_TP = 4


def draw_routes(key, part):
    blocks = TOKENS // TOK_DEV
    half_block = TOK_DEV // 2
    subkeys = jax.random.split(jax.random.fold_in(key, 7), 8)
    common = jax.random.randint(subkeys[0], (), 0, N_GROUPS)
    own_big = jax.random.randint(subkeys[1], (blocks,), 0, N_GROUPS)
    big_group = jnp.where(jnp.arange(blocks) < blocks // 2, common, own_big)
    cut_points = jnp.sort(jax.random.randint(subkeys[2], (blocks, N_GROUPS - 2), 0, half_block + 1), axis=1)
    edges = jnp.concatenate([jnp.zeros((blocks, 1), jnp.int32), cut_points.astype(jnp.int32), jnp.full((blocks, 1), half_block, jnp.int32)], axis=1)
    small_sizes = edges[:, 1:] - edges[:, :-1]
    groups = jnp.arange(N_GROUPS, dtype=jnp.int32)
    offset = (groups[None, :] - big_group[:, None] - 1) % N_GROUPS
    group_sizes = jnp.where(offset == N_GROUPS - 1, half_block, jnp.take_along_axis(small_sizes, jnp.minimum(offset, N_GROUPS - 2), axis=1))
    group_ends = jnp.cumsum(group_sizes, axis=1)
    starts = group_ends - group_sizes
    token_ranks = jnp.argsort(jax.random.randint(subkeys[3], (blocks, TOK_DEV), 0, 1 << 20) * TOK_DEV + jnp.arange(TOK_DEV, dtype=jnp.int32)[None, :], axis=1)
    group_of = jnp.sum((token_ranks[:, :, None] >= group_ends[:, None, :]).astype(jnp.int32), axis=2)
    inner_rank = token_ranks - jnp.take_along_axis(starts, group_of, axis=1)
    first_shift = jax.random.randint(subkeys[4], (blocks, N_GROUPS), 0, PER_GROUP)
    second_step = jax.random.randint(subkeys[5], (blocks, N_GROUPS), 1, PER_GROUP)
    local_order = jnp.argsort(jax.random.randint(subkeys[6], (blocks, N_GROUPS, PER_GROUP), 0, 1 << 20) * PER_GROUP + jnp.arange(PER_GROUP, dtype=jnp.int32), axis=2)
    first_local = (inner_rank + jnp.take_along_axis(first_shift, group_of, axis=1)) % PER_GROUP
    second_local = (first_local + jnp.take_along_axis(second_step, group_of, axis=1)) % PER_GROUP
    group_table = local_order[jnp.arange(blocks)[:, None], group_of]
    local_pair = jnp.take_along_axis(group_table, jnp.stack([first_local, second_local], axis=2), axis=2)
    experts = group_of[:, :, None] * PER_GROUP + local_pair
    return experts.reshape(TOKENS, TOP).astype(jnp.int32)


def steps_of(own_key, extent, shards, least, largest):
    def one(dim, shards_of):
        heights = jax.random.uniform(jax.random.fold_in(jax.random.fold_in(own_key, 6), dim), (shards_of,), jnp.float32, least / len(shards), largest / len(shards))
        return jnp.repeat(jnp.exp(heights), extent[dim] // shards_of).reshape((-1,) + (1,) * (len(extent) - dim - 1))

    loudness = one(*shards[0])
    for cut in shards[1:]:
        loudness = loudness * one(*cut)
    return loudness


def gaussian(key, dims, width, reach, cuts=(), held_as=jnp.bfloat16):
    entries = jax.random.normal(key, dims, jnp.float32) * width
    if len(cuts) > 0:
        entries = steps_of(key, dims, cuts, -0.22, 0.18) * entries
    return jnp.clip(entries, min=-reach, max=reach).astype(held_as)


def setup_inputs(seed: int = 0) -> dict:
    streams_of = jax.random.split(jax.random.key(seed), 8)
    return {
        "prompt": gaussian(streams_of[0], (TOKENS, D), 1.0, 6.0, ((0, 8),)),
        "norm_gain": jnp.clip(1.0 + 0.18 * jax.random.normal(streams_of[1], (D,), jnp.float32), 0.1, 1.9),
        "gate_master": gaussian(streams_of[2], (N_EXPERTS, D, FF), 1.0, 6.0, ((1, 8), (2, 4)), jnp.float32),
        "up_master": gaussian(streams_of[3], (N_EXPERTS, D, FF), 1.0, 6.0, ((1, 8), (2, 4)), jnp.float32),
        "down_master": gaussian(streams_of[4], (N_EXPERTS, D, FF), 1.0, 6.0, ((1, 8), (2, 4)), jnp.float32),
        "routes": draw_routes(jax.random.fold_in(streams_of[7], 71), 0),
        "route_weights": jnp.clip(0.1 + 0.79999997 * jax.random.uniform(streams_of[6], (TOKENS, TOP), jnp.float32) ** steps_of(streams_of[6], (TOKENS, TOP), ((0, 8),), -0.2, 0.2), 0.1, 0.9),
    }


EPS = 1e-06

def reference(prompt, norm_gain, gate_master, up_master, down_master, routes, route_weights):
    gate_new = (norm_gain[None, :, None] * gate_master).astype(jnp.bfloat16)
    up_new = (norm_gain[None, :, None] * up_master).astype(jnp.bfloat16)
    down_new = down_master.astype(jnp.bfloat16)
    prompt_wide = prompt.astype(jnp.float32)
    normed = (prompt_wide * lax.rsqrt(lax.optimization_barrier(jnp.mean(prompt_wide * prompt_wide, axis=-1, keepdims=True)) + EPS)).astype(jnp.bfloat16)
    route_list = routes.reshape(-1).astype(jnp.int32)
    route_hits = (route_list[:, None] == jnp.arange(N_EXPERTS, dtype=jnp.int32)[None, :]).astype(jnp.int32)
    slot_rank = lax.optimization_barrier(jnp.sum((jnp.cumsum(route_hits, axis=0).astype(jnp.int32) - 1) * route_hits, axis=1)).astype(jnp.int32)
    expert_room = TOKENS // TOK_DEV * CAP
    slot_index = (route_list * expert_room + slot_rank).astype(jnp.int32)
    token_of = (jnp.arange(route_list.shape[0], dtype=jnp.int32) // TOP).astype(jnp.int32)
    slot_owner = jnp.zeros((N_EXPERTS * expert_room,), jnp.int32).at[slot_index].set(token_of)

    def expert(operands):
        row_ids, gate_rows, up_rows, down_rows = operands
        picked = normed[row_ids]
        pre_gate = jnp.dot(picked, gate_rows, preferred_element_type=jnp.float32) * D ** (-0.5)
        pre_up = jnp.dot(picked, up_rows, preferred_element_type=jnp.float32) * D ** (-0.5)
        hidden = (jax.nn.silu(pre_gate) * pre_up).astype(jnp.bfloat16)
        hidden_blocks = hidden.astype(jnp.float32).reshape(row_ids.shape[0], N_TP, FF // N_TP)
        down_blocks = down_rows.astype(jnp.float32).reshape(D, N_TP, FF // N_TP)
        partial_value = (jnp.einsum('rnf,dnf->rnd', hidden_blocks, down_blocks) * FF ** (-0.5)).astype(jnp.bfloat16)
        return lax.optimization_barrier(jnp.sum(partial_value.astype(jnp.float32), axis=1)).astype(jnp.bfloat16)
    results = lax.map(expert, (slot_owner.reshape(N_EXPERTS, expert_room), gate_new, up_new, down_new))
    per_choice = results.reshape(N_EXPERTS * expert_room, D)[slot_index].reshape(TOKENS, TOP, D)
    blended = lax.optimization_barrier(jnp.sum(per_choice.astype(jnp.float32) * route_weights[:, :, None], axis=1))
    return (gate_new, up_new, down_new, blended.astype(jnp.bfloat16))
```

```python
import jax
import jax.numpy as jnp
from jax import lax
from jax.sharding import PartitionSpec as P

EPS = 1e-06
CHUNKS = 4
DEPTH = 2


def shift(n, s):
    return [(i, (i + s) % n) for i in range(n)]


def after(values, others):
    if not others:
        return list(values)
    return list(lax.optimization_barrier((tuple(values), tuple(others)))[0])


def per_device(prompt, norm_gain, gate_master, up_master, down_master, routes, route_weights):
    n, ng, nt = lax.axis_size("fs"), lax.axis_size("gr"), lax.axis_size("tp")
    me, mg, mt = lax.axis_index("fs"), lax.axis_index("gr"), lax.axis_index("tp")
    experts, rows, cols = gate_master.shape
    local = experts // n
    blocks = n * ng
    width = blocks * rows
    hidden_units = cols * nt
    tokens = prompt.shape[0]
    room = min(tokens // 2, local * (tokens // 8))

    def piece(master, scale, s, lo_e, num_e, lo_r, num_r):
        start = lax.rem(me + s, n) * local + lo_e
        part = lax.dynamic_slice(master, (start, lo_r, 0), (num_e, num_r, cols))
        if scale:
            part = part * norm_gain[None, lo_r : lo_r + num_r, None]
        return part.astype(jnp.bfloat16)

    history = []

    def over_fs(outgoing, sign=1):
        tied = history[-DEPTH] if len(history) >= DEPTH else []
        flat = [x for s in range(1, n) for x in outgoing[s]]
        flat = after(flat, tied)
        got, at = [list(outgoing[0])], 0
        for s in range(1, n):
            got.append([])
            for _ in outgoing[s]:
                got[s].append(lax.ppermute(flat[at], "fs", shift(n, sign * s)))
                at += 1
        history.append([x for s in range(1, n) for x in got[s]])
        return got

    def over_gr(value):
        return [value] + [lax.ppermute(value, "gr", shift(ng, q)) for q in range(1, ng)]

    def weight_group(master, scale, lo_e, num_e, lo_r, num_r):
        got = over_fs([[piece(master, scale, s, lo_e, num_e, lo_r, num_r)] for s in range(n)])
        return [over_gr(g[0]) for g in got]

    def placed(out, arrived, put):
        for s in range(n):
            for q in range(ng):
                block = lax.rem(mg - q + ng, ng) * n + lax.rem(me - s + n, n)
                out = put(out, arrived[s][q], block)
        return out

    half = max(local // 2, 1)

    def by_experts(master):
        out = jnp.zeros((local, width, cols), jnp.bfloat16)
        for lo in range(0, local, half):
            arrived = weight_group(master, True, lo, half, 0, rows)
            out = placed(
                out,
                arrived,
                lambda o, x, b, lo=lo: lax.dynamic_update_slice(o, x, (lo, b * rows, 0)),
            )
            yield out

    gate_steps = by_experts(gate_master)
    up_steps = by_experts(up_master)
    gate_ready = next(gate_steps)

    wide = prompt.astype(jnp.float32)
    normed = (wide * lax.rsqrt(jnp.mean(wide * wide, axis=-1, keepdims=True) + EPS)).astype(
        jnp.bfloat16
    )
    slab = width // nt
    mine = lax.dynamic_slice_in_dim(normed, mt * slab, slab, 1)
    far = lax.rem(routes // local - me + n, n)
    hit = jnp.any(far[:, :, None] == jnp.arange(n, dtype=jnp.int32)[None, None, :], axis=1)
    order = lax.broadcasted_iota(jnp.int32, (tokens, tokens), 0) >= lax.broadcasted_iota(
        jnp.int32, (tokens, tokens), 1
    )
    rank = (
        jnp.dot(
            order.astype(jnp.bfloat16), hit.astype(jnp.bfloat16), preferred_element_type=jnp.float32
        ).astype(jnp.int32)
        - 1
    )
    slot = jnp.where(hit, rank, -1).T
    pick = (
        slot[:, None, :] == jnp.arange(room, dtype=jnp.int32)[None, :, None]
    ).astype(jnp.bfloat16)
    rows_out = jnp.einsum(
        "srt,td->srd", pick, mine, preferred_element_type=jnp.float32
    ).astype(jnp.bfloat16)
    inner = lax.rem(routes, local)
    share = jnp.sum(
        jnp.where(
            (far[:, :, None, None] == jnp.arange(n, dtype=jnp.int32)[None, None, :, None])
            & (inner[:, :, None, None] == jnp.arange(local, dtype=jnp.int32)[None, None, None, :]),
            route_weights[:, :, None, None],
            0.0,
        ),
        axis=1,
    )
    share_out = jnp.einsum(
        "srt,tse->ser", pick.astype(jnp.float32), share, precision=lax.Precision.HIGHEST
    )
    arrived = over_fs([[rows_out[s], share_out[s]] for s in range(n)])
    tok_slab = jnp.stack([a[0] for a in arrived])
    shares = jnp.stack([a[1] for a in arrived])
    shares = jnp.transpose(shares, (0, 2, 1)).reshape(n * room, local)
    tok = lax.all_gather(tok_slab.reshape(n * room, slab), "tp", axis=1, tiled=True)

    for gate_ready in gate_steps:
        pass
    for up_ready in up_steps:
        pass
    pre_gate = jnp.einsum(
        "rd,edf->ref", tok, gate_ready, preferred_element_type=jnp.float32
    ) * width ** (-0.5)
    pre_up = jnp.einsum(
        "rd,edf->ref", tok, up_ready, preferred_element_type=jnp.float32
    ) * width ** (-0.5)
    weight = shares[:, :, None]
    hidden = jnp.where(weight != 0, jax.nn.silu(pre_gate) * pre_up * weight, 0.0).astype(
        jnp.bfloat16
    )

    step = rows // CHUNKS
    per_tp = blocks // nt
    down_parts, answers = [], []
    bits = []
    b = 1
    while b < nt:
        bits.append(b)
        b *= 2
    for c in range(CHUNKS):
        arrived = weight_group(down_master, False, 0, local, c * step, step)
        part = placed(
            jnp.zeros((local, blocks, step, cols), jnp.bfloat16),
            arrived,
            lambda o, x, b: lax.dynamic_update_slice(o, x[:, None], (0, b, 0, 0)),
        )
        down_parts.append(part)
        value = (
            jnp.einsum("ref,enjf->rnj", hidden, part, preferred_element_type=jnp.float32)
            * hidden_units ** (-0.5)
        ).astype(jnp.bfloat16)
        value = value.reshape(n * room, nt, per_tp * step)
        span = nt
        for bit in bits:
            my_bit = lax.rem(mt // bit, 2)
            view = value.reshape(n * room, span // 2, 2, per_tp * step)
            keep = lax.dynamic_index_in_dim(view, my_bit, 2, keepdims=False)
            give = lax.dynamic_index_in_dim(view, 1 - my_bit, 2, keepdims=False)
            got = lax.ppermute(give, "tp", [(i, i ^ bit) for i in range(nt)])
            value = (keep.astype(jnp.float32) + got.astype(jnp.float32)).astype(jnp.bfloat16)
            span //= 2
        value = value.reshape(n, room, per_tp * step)
        back = [value[0]] + [
            lax.ppermute(value[s], "fs", shift(n, -s)) for s in range(1, n)
        ]
        answers.append(
            jnp.einsum(
                "srt,srd->td", pick, jnp.stack(back), preferred_element_type=jnp.float32
            ).astype(jnp.bfloat16)
        )
    down_ready = jnp.stack(down_parts, axis=2).reshape(local, width, cols)
    blended = jnp.stack(
        [a.reshape(tokens, per_tp, step) for a in answers], axis=2
    ).reshape(tokens, per_tp * rows)
    return gate_ready, up_ready, down_ready, blended


def solution(mesh):
    weights = P(None, ("gr", "fs"), "tp")
    split = P(("gr", "fs"), None)
    ready = P("fs", None, "tp")
    return jax.shard_map(
        per_device,
        mesh=mesh,
        in_specs=(split, P(("gr", "fs")), weights, weights, weights, split, split),
        out_specs=(ready, ready, ready, P(("gr", "fs"), "tp")),
        check_vma=False,
    )
```
